256 devices in a mesh: ep: 64 (over z, y, core), tp: 4 (over x).
Axes of the slice: x: 4, y: 4, z: 8, core: 2. Of those that a mesh axis runs over, the one named last changes fastest.
Arguments:
- mixer_input: bfloat16 [32768, 2048], P(('ep', 'tp')), may hold values from -6 to 6
- expert_input: bfloat16 [32768, 2048], P(('ep', 'tp')), may hold values from -6 to 6
- mixer_gain: float32 [2048], replicated, may hold values from 0.1 to 1.9
- expert_gain: float32 [2048], replicated, may hold values from 0.1 to 1.9
- query_weight: bfloat16 [2048, 1024], P(None, 'tp'), may hold values from -0.125 to 0.125
- key_weight: bfloat16 [2048, 1024], P(None, 'tp'), may hold values from -0.125 to 0.125
- value_weight: bfloat16 [2048, 1024], P(None, 'tp'), may hold values from -0.125 to 0.125
- out_weight: bfloat16 [1024, 2048], P('tp'), may hold values from -0.1875 to 0.1875
- decay_rate: float32 [8], P('tp'), may hold values from 0 to 0.12
- routing: int32 [32768, 4], P('ep'), may hold values from 0 to 63, all different within a row; in each aligned block of 128 rows (0 to 127, 128 to 255, ...) at most 12 rows name the same one
- route_weight: float32 [32768, 4], P('ep'), may hold values from 0.2 to 1
- gate_weight: bfloat16 [64, 2048, 1024], P('ep', None, 'tp'), may hold values from -0.125 to 0.125
- up_weight: bfloat16 [64, 2048, 1024], P('ep', None, 'tp'), may hold values from -0.125 to 0.125
- down_weight: bfloat16 [64, 1024, 2048], P('ep', None, 'tp'), may hold values from -0.1875 to 0.1875
- shared_gate: bfloat16 [2048, 512], P(None, 'tp'), may hold values from -0.125 to 0.125
- shared_up: bfloat16 [2048, 512], P(None, 'tp'), may hold values from -0.125 to 0.125
- shared_down: bfloat16 [512, 2048], P(None, 'tp'), may hold values from -0.25 to 0.25
Outputs:
- mixer_output: float32 [32768, 2048], P(('ep', 'tp'))
- expert_output: float32 [32768, 2048], P('ep', 'tp')
The draws below stay inside these ranges and needn't reach their ends.
Inputs may be any that keep to these rules, and one draw needn't show every extreme that they name: `routing`: each row names 4 different experts. In each aligned block of 128 rows, no expert is named by more than 12 rows, and in some blocks one expert is named by exactly 12 rows.
All inputs are finite; a program needn't handle non-finite values.
Results may differ from the reference program's by a relative error of at most 0.0095.
Values may be sent and summed in bfloat16 or wider, within the bound.
A program may use at most 128 MiB of HBM per device.

```python
import math
import jax
import jax.numpy as jnp
import numpy as np
from jax import lax

D = 2048
HEADS = 8
HD = 128
F = 1024
FS = 512
K = 4
BLK = 64
R = 128
TOKENS = 32768
EXPERTS = 64
CAP = 12
N_EP = 64
N_TP = 4


def draw_decay_rate(key, part):
    order_key = jax.random.fold_in(key, 11)
    slow_key = jax.random.fold_in(key, 12)
    fast_key = jax.random.fold_in(key, 13)
    ranking = jax.random.permutation(order_key, HEADS)
    fast_count = HEADS // 2
    is_fast = ranking < fast_count
    slow_rate = jnp.exp(jax.random.uniform(slow_key, (HEADS,), jnp.float32, math.log(0.05), 0.0)) * (math.log(10.0) / TOKENS)
    quick_decay_rate = jax.random.uniform(fast_key, (HEADS,), jnp.float32, 0.05, 0.12)
    return jnp.where(is_fast, quick_decay_rate, slow_rate).astype(jnp.float32)


def block_levels(key, extent, split, low, top_value):
    gain, own = 1.0, jax.random.fold_in(key, 6)
    for position, shards_of in split:
        heights = jnp.exp(jax.random.uniform(jax.random.fold_in(own, position), (shards_of,), jnp.float32, low / len(split), top_value / len(split)))
        gain = gain * jnp.repeat(heights, extent[position] // shards_of).reshape([-1 if axis == position else 1 for axis in range(len(extent))])
    return gain


def assign_block(rng, own, number, rows, count, top, bound, skew):
    order = jax.random.permutation(rng, count)
    heavy_load, ordinary = shares(count, rows * top, bound, skew, True), shares(count, rows * top, bound, skew, False)
    places = jnp.arange(count)

    def named(tallies, rotation):
        used = int((tallies > 0).sum())
        fixed = max(1, used // 4)
        moved = fixed + (places - fixed + rotation * (used - fixed)) % max(1, count - fixed)
        return jnp.zeros((count,), jnp.int32).at[order[jnp.where(places < fixed, places, moved)]].set(jnp.asarray(tallies, jnp.int32))

    tallies = jnp.where(number % 4 == 0, named(heavy_load, number // 4), named(ordinary, number - number // 4 - 1))
    mixed = jax.random.permutation(jax.random.fold_in(own, 3), count)
    source_of, receiver = mixed[0:count // 2 * 2:2], mixed[1:count // 2 * 2:2]
    margin = jnp.minimum(tallies[source_of] - 1, bound - tallies[receiver]) // 2
    margin = jnp.where((source_of == order[0]) | (receiver == order[0]) | (tallies[receiver] == 0), 0, jnp.maximum(margin, 0))
    moved = jax.random.randint(jax.random.fold_in(own, 4), (count // 2,), 0, 1 << 20) % (margin + 1)
    tallies = tallies.at[source_of].add(-moved).at[receiver].add(moved)
    items = jnp.searchsorted(jnp.cumsum(tallies), jnp.arange(rows * top), side="right").astype(jnp.int32)
    grid = items.reshape(top, rows).T
    grid = grid[jax.random.permutation(jax.random.fold_in(own, 1), rows)]
    rotation = jax.random.randint(jax.random.fold_in(own, 2), (rows, 1), 0, top)
    return jnp.take_along_axis(grid, (jnp.arange(top)[None, :] + rotation) % top, axis=1)


def shares(number_of, total, bound, skew, full):
    portions = [(1 << 20) // math.isqrt(grade ** skew) + 1 for grade in range(1, number_of + 1)]
    largest = bound if full else min(bound, max(-(-total // number_of), total * portions[0] // sum(portions)))
    least = 1 if total - largest >= number_of - 1 else 0
    counts, rest = [largest] + [least] * (number_of - 1), total - largest - least * (number_of - 1)
    while rest > 0:
        movable = [i for i in range(1, number_of) if counts[i] < largest] or [i for i in range(1, number_of) if counts[i] < bound]
        mass, budget = sum([portions[i] for i in movable]), rest
        for i in movable:
            more = min(bound - counts[i], max(1, budget * portions[i] // mass), rest)
            counts[i] = counts[i] + more
            rest = rest - more
    return np.array(counts)


def gaussian(key, dims, spread, most, shards=(), kind=jnp.bfloat16):
    array = jax.random.normal(key, dims, jnp.float32) * spread
    if len(shards) > 0:
        array = block_levels(key, dims, shards, -0.22, 0.18) * array
    return jnp.clip(array, min=-most, max=most).astype(kind)


def setup_inputs(seed: int = 0) -> dict:
    key_list = jax.random.split(jax.random.key(seed), 18)
    mixer_input = gaussian(key_list[0], (TOKENS, D), 1.0, 6.0, ((0, 256),))
    expert_input = gaussian(key_list[1], (TOKENS, D), 1.0, 6.0, ((0, 256),))
    mixer_gain = jnp.clip(1.0 + 0.18 * jax.random.normal(key_list[2], (D,), jnp.float32), 0.1, 1.9)
    expert_gain = jnp.clip(1.0 + 0.18 * jax.random.normal(key_list[3], (D,), jnp.float32), 0.1, 1.9)
    query_weight = gaussian(key_list[4], (D, HEADS * HD), D ** -0.5, 0.125, ((1, 4),))
    key_weight = gaussian(key_list[5], (D, HEADS * HD), D ** -0.5, 0.125, ((1, 4),))
    value_weight = gaussian(key_list[6], (D, HEADS * HD), D ** -0.5, 0.125, ((1, 4),))
    out_weight = gaussian(key_list[7], (HEADS * HD, D), (HEADS * HD) ** -0.5, 0.1875, ((0, 4),))
    decay_rate = draw_decay_rate(jax.random.fold_in(key_list[17], 71), 0)
    routing_keys = jax.random.split(jax.random.fold_in(key_list[9], 1), TOKENS // R)
    routing_turns = jax.random.permutation(jax.random.fold_in(key_list[9], 3), TOKENS // R)
    routing = jax.vmap(lambda own, number: assign_block(jax.random.fold_in(key_list[9], 2), own, number, R, EXPERTS, K, CAP, 1))(routing_keys, routing_turns).reshape((TOKENS, K))
    route_weight = jnp.clip(0.2 + 0.8 * jax.random.uniform(key_list[10], (TOKENS, K), jnp.float32) ** block_levels(key_list[10], (TOKENS, K), ((0, 64),), -0.2, 0.2), 0.2, 1.0)
    gate_weight = gaussian(key_list[11], (EXPERTS, D, F), D ** -0.5, 0.125, ((0, 64), (2, 4)))
    up_weight = gaussian(key_list[12], (EXPERTS, D, F), D ** -0.5, 0.125, ((0, 64), (2, 4)))
    down_weight = gaussian(key_list[13], (EXPERTS, F, D), F ** -0.5, 0.1875, ((0, 64), (2, 4)))
    shared_gate = gaussian(key_list[14], (D, FS), D ** -0.5, 0.125, ((1, 4),))
    shared_up = gaussian(key_list[15], (D, FS), D ** -0.5, 0.125, ((1, 4),))
    shared_down = gaussian(key_list[16], (FS, D), FS ** -0.5, 0.25, ((1, 4),))
    return dict(mixer_input=mixer_input, expert_input=expert_input, mixer_gain=mixer_gain, expert_gain=expert_gain, query_weight=query_weight, key_weight=key_weight, value_weight=value_weight, out_weight=out_weight, decay_rate=decay_rate, routing=routing, route_weight=route_weight, gate_weight=gate_weight, up_weight=up_weight, down_weight=down_weight, shared_gate=shared_gate, shared_up=shared_up, shared_down=shared_down)


NORM_EPS = 1e-06
ROPE_BASE = 10000.0
EXACT_MATMUL = lax.Precision.HIGHEST

def norm_rows(inputs, gain_vector):
    values = inputs.astype(jnp.float32)
    scaled = values * lax.rsqrt(lax.optimization_barrier(jnp.mean(values * values, axis=-1, keepdims=True)) + NORM_EPS)
    return (scaled * gain_vector.astype(jnp.float32)).astype(jnp.bfloat16)

def rotate(head_rows, positions):
    head_size = head_rows.shape[-1]
    inverse = ROPE_BASE ** (-jnp.arange(0, head_size, 2, dtype=jnp.float32) / head_size)
    angles = positions[:, None] * inverse[None, :]
    cosine = jnp.cos(angles)[:, None, :]
    sine_part = jnp.sin(angles)[:, None, :]
    front_half = head_rows[..., :head_size // 2]
    behind = head_rows[..., head_size // 2:]
    return jnp.concatenate([front_half * cosine - behind * sine_part, front_half * sine_part + behind * cosine], axis=-1)

def project(inputs, weight):
    product = jnp.dot(inputs, weight, preferred_element_type=jnp.float32).astype(jnp.bfloat16)
    product = lax.optimization_barrier(product)
    return product.astype(jnp.float32).reshape(inputs.shape[0], HEADS, HD)

def retention_scan(query_heads, key_heads, value_heads, decay_rates):
    length = query_heads.shape[0]
    blocks = length // BLK
    log_gamma = -decay_rates.astype(jnp.float32)
    inner_pos = jnp.arange(BLK, dtype=jnp.float32)
    offsets = inner_pos[:, None] - inner_pos[None, :]
    inside_block_output = jnp.where(offsets >= 0, jnp.exp(log_gamma[:, None, None] * jnp.maximum(offsets, 0.0)), 0.0)
    key_scale = jnp.exp(log_gamma[None, :] * (BLK - 1.0 - inner_pos)[:, None])
    query_scale = jnp.exp(log_gamma[None, :] * (inner_pos + 1.0)[:, None])
    through = jnp.exp(log_gamma * BLK)

    def advance(carried, block_in):
        query_block_slice, key_block_slice, v_block = block_in
        attention_scores = jnp.einsum('ayr,iyr->yai', query_block_slice, key_block_slice, precision=EXACT_MATMUL) * inside_block_output
        nearby = jnp.einsum('hcm,mhe->che', attention_scores, v_block, precision=EXACT_MATMUL)
        distant = jnp.einsum('chd,hde->che', query_block_slice * query_scale[:, :, None], carried, precision=EXACT_MATMUL)
        update = jnp.einsum('chd,che->hde', key_block_slice * key_scale[:, :, None], v_block, precision=EXACT_MATMUL)
        return (through[:, None, None] * carried + update, nearby + distant)
    blocked = (blocks, BLK, HEADS, HD)
    _, outputs = lax.scan(advance, jnp.zeros((HEADS, HD, HD), jnp.float32), (query_heads.reshape(blocked), key_heads.reshape(blocked), value_heads.reshape(blocked)))
    return outputs.reshape(length, HEADS, HD)

def reference(mixer_input, expert_input, mixer_gain, expert_gain, query_weight, key_weight, value_weight, out_weight, decay_rate, routing, route_weight, gate_weight, up_weight, down_weight, shared_gate, shared_up, shared_down):
    mixer_rows = norm_rows(mixer_input, mixer_gain)
    positions = jnp.arange(TOKENS, dtype=jnp.float32)
    query_heads = rotate(project(mixer_rows, query_weight), positions) * HD ** (-0.5)
    key_heads = rotate(project(mixer_rows, key_weight), positions)
    value_heads = project(mixer_rows, value_weight)
    retained = retention_scan(query_heads, key_heads, value_heads, decay_rate)
    normed = retained * lax.rsqrt(lax.optimization_barrier(jnp.mean(retained * retained, axis=-1, keepdims=True)) + NORM_EPS)
    mixed_heads = normed.astype(jnp.bfloat16).reshape(TOKENS, HEADS * HD)
    group_width = HEADS * HD // N_TP
    summed_out = jnp.zeros((TOKENS, D), jnp.float32)
    for group_id in range(N_TP):
        partial_out = jnp.dot(mixed_heads[:, group_id * group_width:(group_id + 1) * group_width], out_weight[group_id * group_width:(group_id + 1) * group_width], preferred_element_type=jnp.float32).astype(jnp.bfloat16)
        summed_out = summed_out + lax.optimization_barrier(partial_out).astype(jnp.float32)
    mixer_output = summed_out
    expert_rows = norm_rows(expert_input, expert_gain)
    assigned = TOKENS * K
    chosen = routing.reshape(assigned).astype(jnp.int32)
    onehot = (chosen[:, None] == jnp.arange(EXPERTS, dtype=jnp.int32)[None, :]).astype(jnp.int32)
    ranks = lax.optimization_barrier(jnp.sum((jnp.cumsum(onehot, axis=0) - onehot) * onehot, axis=1)).astype(jnp.int32)
    owners = (jnp.arange(assigned, dtype=jnp.int32) // K + 1).astype(jnp.int32)
    room_size = N_EP * N_TP * CAP
    owner_table = jnp.zeros((EXPERTS, room_size), jnp.int32).at[chosen, ranks].set(owners)
    weight_table = jnp.zeros((EXPERTS, room_size), jnp.float32).at[chosen, ranks].set(route_weight.reshape(assigned).astype(jnp.float32))
    padded = jnp.concatenate([jnp.zeros((1, D), jnp.bfloat16), expert_rows], axis=0)

    def one_expert(summed, inputs):
        owner_ids, scales, gate_part, up_part, down_part = inputs
        picked = padded[owner_ids]
        hidden = (jax.nn.silu(jnp.dot(picked, gate_part, preferred_element_type=jnp.float32)) * jnp.dot(picked, up_part, preferred_element_type=jnp.float32)).astype(jnp.bfloat16)
        result = jnp.dot(hidden, down_part, preferred_element_type=jnp.float32).astype(jnp.bfloat16)
        result = lax.optimization_barrier(result).astype(jnp.float32)
        return (summed.at[owner_ids].add(result * scales[:, None]), None)
    summed, _ = lax.scan(one_expert, jnp.zeros((TOKENS + 1, D), jnp.float32), (owner_table, weight_table, gate_weight, up_weight, down_weight))
    shared_hidden = (jax.nn.silu(jnp.dot(expert_rows, shared_gate, preferred_element_type=jnp.float32)) * jnp.dot(expert_rows, shared_up, preferred_element_type=jnp.float32)).astype(jnp.bfloat16)
    shared_result = jnp.dot(shared_hidden, shared_down, preferred_element_type=jnp.float32)
    expert_output = summed[1:] + shared_result
    return (mixer_output, expert_output)
```

```python
import jax
import jax.numpy as jnp
from jax import lax
from jax.sharding import Mesh
from jax.sharding import PartitionSpec as P

HD = 128
BLK = 64
CAP = 12
EP = ("ep_0", "ep_1", "ep_2")
PLANE = ("ep_1", "ep_2")
EP_TP = ("ep_0", "ep_1", "ep_2", "tp")
NORM_EPS = 1e-06
ROPE_BASE = 10000.0
EXACT_MATMUL = lax.Precision.HIGHEST


def norm_rows(inputs, gain_vector):
    values = inputs.astype(jnp.float32)
    scaled = values * lax.rsqrt(jnp.mean(values * values, axis=-1, keepdims=True) + NORM_EPS)
    return (scaled * gain_vector).astype(jnp.bfloat16)


def rotate(head_rows, positions):
    head_size = head_rows.shape[-1]
    inverse = ROPE_BASE ** (-jnp.arange(0, head_size, 2, dtype=jnp.float32) / head_size)
    angles = positions[:, None] * inverse[None, :]
    cosine = jnp.cos(angles)[:, None, :]
    sine_part = jnp.sin(angles)[:, None, :]
    front_half = head_rows[..., : head_size // 2]
    behind = head_rows[..., head_size // 2 :]
    return jnp.concatenate(
        [front_half * cosine - behind * sine_part, front_half * sine_part + behind * cosine],
        axis=-1,
    )


def project(inputs, weight, head_total):
    product = jnp.dot(inputs, weight, preferred_element_type=jnp.float32).astype(jnp.bfloat16)
    product = lax.optimization_barrier(product)
    return product.astype(jnp.float32).reshape(inputs.shape[0], head_total, -1)


def entering_state(summary, log_gamma, length):
    planes, members = lax.axis_size("ep_0"), lax.axis_size(PLANE)
    z, j = lax.axis_index("ep_0"), lax.axis_index(PLANE)
    heads = summary.shape[0]
    per_head = members // heads
    sliced = summary.reshape(members, HD // per_head, HD)
    theirs = lax.all_to_all(sliced, PLANE, split_axis=0, concat_axis=0, tiled=True)
    rate = jnp.where(jnp.arange(heads) == j // per_head, log_gamma, 0.0).sum() * length
    spots = jnp.arange(members, dtype=jnp.float32)
    total = jnp.sum(jnp.exp(rate * (members - 1.0 - spots))[:, None, None] * theirs, axis=0)
    totals = lax.all_gather(total, "ep_0")
    plane_ids = jnp.arange(planes)
    before = jnp.where(
        plane_ids < z, jnp.exp(rate * members * jnp.maximum(z - 1 - plane_ids, 0)), 0.0
    )
    passed = jnp.sum(before[:, None, None] * totals, axis=0)
    gaps = spots[:, None] - 1.0 - spots[None, :]
    mix = jnp.where(gaps >= 0, jnp.exp(rate * jnp.maximum(gaps, 0.0)), 0.0)
    inside = jnp.einsum("ij,jab->iab", mix, theirs, precision=EXACT_MATMUL)
    mine = inside + jnp.exp(rate * spots)[:, None, None] * passed[None]
    back = lax.all_to_all(mine, PLANE, split_axis=0, concat_axis=0, tiled=True)
    return back.reshape(summary.shape)


def retain_local(query_heads, key_heads, value_heads, decay_rates):
    length, head_total, head_size = query_heads.shape
    blocks = length // BLK
    log_gamma = -decay_rates
    inner_pos = jnp.arange(BLK, dtype=jnp.float32)
    offsets = inner_pos[:, None] - inner_pos[None, :]
    inside_block_output = jnp.where(
        offsets >= 0, jnp.exp(log_gamma[:, None, None] * jnp.maximum(offsets, 0.0)), 0.0
    )
    key_scale = jnp.exp(log_gamma[None, :] * (BLK - 1.0 - inner_pos)[:, None])
    query_scale = jnp.exp(log_gamma[None, :] * (inner_pos + 1.0)[:, None])
    blocked = (blocks, BLK, head_total, head_size)
    q_blocks = query_heads.reshape(blocked)
    k_blocks = key_heads.reshape(blocked)
    v_blocks = value_heads.reshape(blocked)
    block_states = jnp.einsum(
        "nchd,nche->nhde", k_blocks * key_scale[None, :, :, None], v_blocks, precision=EXACT_MATMUL
    )
    block_offset_rows = jnp.arange(blocks, dtype=jnp.float32)
    to_end = jnp.exp(log_gamma[None, :] * BLK * (blocks - 1.0 - block_offset_rows)[:, None])
    summary = jnp.einsum("nh,nhde->hde", to_end, block_states, precision=EXACT_MATMUL)
    incoming = entering_state(summary, log_gamma, float(length))
    attention_scores = (
        jnp.einsum("nchd,nmhd->nhcm", q_blocks, k_blocks, precision=EXACT_MATMUL)
        * inside_block_output[None]
    )
    nearby = jnp.einsum("nhcm,nmhe->nche", attention_scores, v_blocks, precision=EXACT_MATMUL)
    block_gaps = block_offset_rows[:, None] - 1.0 - block_offset_rows[None, :]
    carry_mix = jnp.where(
        block_gaps >= 0, jnp.exp(log_gamma[:, None, None] * BLK * jnp.maximum(block_gaps, 0.0)), 0.0
    )
    entering = jnp.einsum("hbj,jhde->bhde", carry_mix, block_states, precision=EXACT_MATMUL)
    entering = (
        entering
        + jnp.exp(log_gamma[None, :] * BLK * block_offset_rows[:, None])[:, :, None, None]
        * incoming[None]
    )
    distant = jnp.einsum(
        "bchd,bhde->bche",
        q_blocks * query_scale[None, :, :, None],
        entering,
        precision=EXACT_MATMUL,
    )
    retained = (nearby + distant).reshape(length, head_total, head_size)
    normed = retained * lax.rsqrt(jnp.mean(retained * retained, axis=-1, keepdims=True) + NORM_EPS)
    return normed.astype(jnp.bfloat16).reshape(length, head_total * head_size)


def shards(
    mixer_input,
    expert_input,
    mixer_gain,
    expert_gain,
    query_weight,
    key_weight,
    value_weight,
    out_weight,
    decay_rate,
    routing,
    route_weight,
    gate_weight,
    up_weight,
    down_weight,
    shared_gate,
    shared_up,
    shared_down,
):
    own_count, width = mixer_input.shape
    tp_index = lax.axis_index("tp")
    experts = lax.axis_size(EP)

    own_mixer = norm_rows(mixer_input, mixer_gain)
    own_rows = norm_rows(expert_input, expert_gain)
    mixer_rows = lax.all_gather(own_mixer, "tp", axis=0, tiled=True)
    gates, ups, downs = (
        lax.all_gather(w[0], "tp") for w in (gate_weight, up_weight, down_weight)
    )
    expert_rows = lax.all_gather(own_rows, "tp", axis=0, tiled=True)

    routes = lax.dynamic_slice_in_dim(routing, tp_index * own_count, own_count, 0)
    scales = lax.dynamic_slice_in_dim(route_weight, tp_index * own_count, own_count, 0)
    hits = routes[:, :, None] == jnp.arange(experts, dtype=jnp.int32)[None, None, :]
    member = jnp.any(hits, axis=1)
    weight = jnp.sum(jnp.where(hits, scales[:, :, None], 0.0), axis=1)
    rows = jnp.arange(own_count)
    lower = (rows[None, :] < rows[:, None]).astype(jnp.bfloat16)
    rank = jnp.dot(lower, member.astype(jnp.bfloat16), preferred_element_type=jnp.float32)
    rank = jnp.where(member, rank, -1.0)
    slots = jnp.arange(CAP, dtype=jnp.float32)
    picks = rank.T[:, None, :] == slots[None, :, None]
    sent = jnp.dot(
        picks.astype(jnp.bfloat16).reshape(experts * CAP, own_count),
        own_rows,
        preferred_element_type=jnp.float32,
    ).astype(jnp.bfloat16)
    arrived = lax.all_to_all(sent, EP, split_axis=0, concat_axis=0, tiled=True)

    group_count = mixer_rows.shape[0]
    head_total = decay_rate.shape[0]
    positions = (
        lax.axis_index(EP) * group_count + jnp.arange(group_count, dtype=jnp.int32)
    ).astype(jnp.float32)
    query_heads = rotate(project(mixer_rows, query_weight, head_total), positions) * HD ** (-0.5)
    key_heads = rotate(project(mixer_rows, key_weight, head_total), positions)
    value_heads = project(mixer_rows, value_weight, head_total)
    mixed_heads = retain_local(query_heads, key_heads, value_heads, decay_rate)
    mixer_output = lax.psum_scatter(
        jnp.dot(mixed_heads, out_weight, preferred_element_type=jnp.float32).astype(jnp.bfloat16),
        "tp",
        scatter_dimension=0,
        tiled=True,
    ).astype(jnp.float32)

    gate_part = jnp.einsum("sd,tdf->stf", arrived, gates, preferred_element_type=jnp.float32)
    up_part = jnp.einsum("sd,tdf->stf", arrived, ups, preferred_element_type=jnp.float32)
    hidden = (jax.nn.silu(gate_part) * up_part).astype(jnp.bfloat16).reshape(arrived.shape[0], -1)
    results = jnp.einsum("sf,tfe->ste", hidden, downs, preferred_element_type=jnp.float32)
    results = results.astype(jnp.bfloat16).reshape(arrived.shape[0], width)
    returned = lax.all_to_all(results, EP, split_axis=0, concat_axis=0, tiled=True)
    spread = jnp.where(picks, weight.T[:, None, :], 0.0).reshape(experts * CAP, own_count)
    high = spread.astype(jnp.bfloat16)
    low = (spread - high.astype(jnp.float32)).astype(jnp.bfloat16)
    summed = jnp.einsum("st,sd->td", high, returned, preferred_element_type=jnp.float32)
    summed = summed + jnp.einsum("st,sd->td", low, returned, preferred_element_type=jnp.float32)
    turned = lax.all_to_all(summed, "tp", split_axis=1, concat_axis=0, tiled=True)

    shared_hidden = (
        jax.nn.silu(jnp.dot(expert_rows, shared_gate, preferred_element_type=jnp.float32))
        * jnp.dot(expert_rows, shared_up, preferred_element_type=jnp.float32)
    ).astype(jnp.bfloat16)
    full_shared = lax.all_gather(shared_hidden, "tp", axis=1, tiled=True)
    shared_result = jnp.dot(full_shared, shared_down, preferred_element_type=jnp.float32)
    return (mixer_output, turned + shared_result)


def solution(mesh):
    finer = Mesh(mesh.devices.reshape(8, 4, 2, mesh.shape["tp"]), ("ep_0", "ep_1", "ep_2", "tp"))
    placed = (
        P(EP_TP, None),
        P(EP_TP, None),
        P(),
        P(),
        P(None, "tp"),
        P(None, "tp"),
        P(None, "tp"),
        P("tp", None),
        P("tp"),
        P(EP, None),
        P(EP, None),
        P(EP, None, "tp"),
        P(EP, None, "tp"),
        P(EP, None, "tp"),
        P(None, "tp"),
        P(None, "tp"),
        P(None, "tp"),
    )
    return jax.shard_map(
        shards,
        mesh=finer,
        in_specs=placed,
        out_specs=(P(EP_TP, None), P(EP, "tp")),
        check_vma=False,
    )
```
